32 devices in a mesh: sp: 8 (over z, y), tp: 4 (over x, core).
Axes of the slice: x: 2, y: 2, z: 4, core: 2. Of those that a mesh axis runs over, the one named last changes fastest.
Arguments:
- skip_stream_vector: bfloat16 [8192, 2048], P(('sp', 'tp')), may hold values from -6 to 6
- probe_preactivation: bfloat16 [8192, 1024], P('sp', 'tp'), may hold values from -6 to 6
- retention_preactivation: bfloat16 [8192, 1024], P('sp', 'tp'), may hold values from -4.5 to 4.5
- content_vector: bfloat16 [8192, 1024], P('sp', 'tp'), may hold values from -6 to 6
- emission_preactivation: bfloat16 [8192, 1024], P('sp', 'tp'), may hold values from -6 to 6
- retention_slack: float32 [1024], P('tp'), may hold values from 0 to 0.12
- surge_rate: float32 [8192, 1024], P('sp', 'tp'), may hold values from -1.2 to 0
- subspace_scaling_factor: float32 [1024], P('tp'), may hold values from 0.1 to 1.9
- emission_matrix: bfloat16 [1024, 2048], replicated, may hold values from -0.1875 to 0.1875
- mlp_scaling_factor: float32 [2048], replicated, may hold values from 0.1 to 1.9
- switch_matrix: bfloat16 [2048, 5632], P('sp', 'tp'), may hold values from -0.125 to 0.125
- expansion_matrix: bfloat16 [2048, 5632], P('sp', 'tp'), may hold values from -0.125 to 0.125
- contraction_matrix: bfloat16 [5632, 2048], P('tp', 'sp'), may hold values from -0.078125 to 0.078125
Outputs:
- stream_out: bfloat16 [8192, 2048], P(('sp', 'tp'))
The draws below stay inside these ranges and needn't reach their ends.
All inputs are finite; a program needn't handle non-finite values.
Results may differ from the reference program's by a relative error of at most 0.017.
Values may be sent and summed in bfloat16 or wider, within the bound.
A program may use at most 128 MiB of HBM per device.

```python
import jax
import jax.numpy as jnp
from jax import lax

D = 2048
HEADS = 8
HEAD_DIM = 128
FF = 5632
BLOCK = 64
TOK_DEV = 1024
D_HGRN = 1024
TOKENS = 8192
N_TP = 4


def draw_retention_slack(key, part):
    first_key, second_key, third_key = jax.random.split(jax.random.fold_in(key, 11), 3)
    ranking = jax.random.permutation(first_key, HEADS)
    slow_heads = ranking < HEADS // 2
    slow_gap = jnp.exp(jax.random.uniform(second_key, (HEADS, HEAD_DIM), jnp.float32, jnp.log(0.2), jnp.log(0.8))) / TOKENS
    fast_gap = jnp.exp(jax.random.uniform(third_key, (HEADS, HEAD_DIM), jnp.float32, jnp.log(0.04), jnp.log(0.12)))
    chosen = jnp.where(slow_heads[:, None], slow_gap, fast_gap)
    return jnp.minimum(chosen, 0.12).reshape(HEADS * HEAD_DIM)


def draw_retention_preactivation(key, part):
    first_key, second_key = jax.random.split(jax.random.fold_in(key, 21))
    noise = jnp.clip(0.8 * jax.random.normal(first_key, (TOKENS, HEADS * HEAD_DIM), jnp.float32), -3.0, 3.0)
    offsets = jax.random.uniform(second_key, (TOKENS // TOK_DEV, HEADS), jnp.float32, -1.2, 1.2)
    spread_rows = jnp.repeat(jnp.repeat(offsets, TOK_DEV, axis=0), HEAD_DIM, axis=1)
    return (noise + spread_rows).astype(jnp.bfloat16)


def draw_surge_rate(key, part):
    first_key, second_key = jax.random.split(jax.random.fold_in(key, 31))
    positions = jax.random.randint(first_key, (2, HEADS), 0, TOKENS)
    strength = jnp.log(jax.random.uniform(second_key, (2, HEADS), jnp.float32, 0.55, 0.8))
    places = jnp.arange(TOKENS, dtype=jnp.int32)[:, None, None]
    hits = jnp.sum(jnp.where(places == positions[None, :, :], strength[None, :, :], 0.0), axis=1)
    return jnp.repeat(hits, HEAD_DIM, axis=1)


def levels(rng, shape, pieces, low, largest):
    loudness, own = 1.0, jax.random.fold_in(rng, 6)
    for position, shards_of in pieces:
        draws = jnp.exp(jax.random.uniform(jax.random.fold_in(own, position), (shards_of,), jnp.float32, low / len(pieces), largest / len(pieces)))
        loudness = loudness * jnp.repeat(draws, shape[position] // shards_of).reshape([-1 if axis == position else 1 for axis in range(len(shape))])
    return loudness


def normal_values(own_key, extent, width, limit, shards=(), kind=jnp.bfloat16):
    drawn = width * jax.random.normal(own_key, extent, jnp.float32)
    if shards:
        drawn = drawn * levels(own_key, extent, shards, -0.22, 0.18)
    return jnp.clip(drawn, -limit, limit).astype(kind)


def setup_inputs(seed: int = 0) -> dict:
    key_of = jax.random.split(jax.random.key(seed), 14)
    return {
        "skip_stream_vector": normal_values(key_of[0], (TOKENS, D), 1.0, 6.0, ((0, 32),)),
        "probe_preactivation": normal_values(key_of[1], (TOKENS, D_HGRN), 1.0, 6.0, ((0, 8), (1, 4))),
        "retention_preactivation": draw_retention_preactivation(jax.random.fold_in(key_of[13], 71), 0),
        "content_vector": normal_values(key_of[3], (TOKENS, D_HGRN), 1.0, 6.0, ((0, 8), (1, 4))),
        "emission_preactivation": normal_values(key_of[4], (TOKENS, D_HGRN), 1.0, 6.0, ((0, 8), (1, 4))),
        "retention_slack": draw_retention_slack(jax.random.fold_in(key_of[13], 71), 0),
        "surge_rate": draw_surge_rate(jax.random.fold_in(key_of[13], 71), 0),
        "subspace_scaling_factor": jnp.clip(1.0 + 0.18 * jax.random.normal(key_of[7], (D_HGRN,), jnp.float32), 0.1, 1.9),
        "emission_matrix": normal_values(key_of[8], (D_HGRN, D), D_HGRN ** -0.5, 0.1875),
        "mlp_scaling_factor": jnp.clip(1.0 + 0.18 * jax.random.normal(key_of[9], (D,), jnp.float32), 0.1, 1.9),
        "switch_matrix": normal_values(key_of[10], (D, FF), D ** -0.5, 0.125, ((0, 8), (1, 4))),
        "expansion_matrix": normal_values(key_of[11], (D, FF), D ** -0.5, 0.125, ((0, 8), (1, 4))),
        "contraction_matrix": normal_values(key_of[12], (FF, D), FF ** -0.5, 0.078125, ((0, 4), (1, 8))),
    }


EPSILON = 1e-06
TOP_PRECISION = lax.Precision.HIGHEST

def block_step(carry, inputs):
    memory_state, offsets = carry
    query_block, input_gate_block, value_block, log_blk = inputs
    cumulative_decay = jnp.cumsum(log_blk, axis=1)
    length = log_blk.shape[1]
    carried_share = jnp.einsum('eia,eax->eix', query_block * jnp.exp(cumulative_decay), memory_state, precision=TOP_PRECISION)
    middle = cumulative_decay[:, length // 2, :][:, None, :]
    left_side = query_block * jnp.exp(cumulative_decay - middle)
    right_side = input_gate_block * jnp.exp(middle - cumulative_decay)
    causal = (jnp.arange(length)[:, None] >= jnp.arange(length)[None, :])[None, :, :]
    scores = jnp.einsum('htk,hsk->hts', left_side, right_side, precision=TOP_PRECISION)
    scores = jnp.where(causal, scores, 0.0)
    outputs = carried_share + jnp.einsum('hts,hsv->htv', scores, value_block, precision=TOP_PRECISION)
    closing_log_decay = cumulative_decay[:, -1, :]
    updated_memory_state = jnp.exp(closing_log_decay)[:, :, None] * memory_state + jnp.einsum('qnj,qnl->qjl', input_gate_block * jnp.exp(closing_log_decay[:, None, :] - cumulative_decay), value_block, precision=TOP_PRECISION)
    return ((updated_memory_state, offsets + closing_log_decay), (outputs, cumulative_decay + offsets[:, None, :]))

def split_blocks(values, heads_here):
    count = values.shape[0]
    return values.reshape(count // BLOCK, BLOCK, heads_here, HEAD_DIM).transpose(0, 2, 1, 3)

def admission_source_matrix(probe_preactivation, retention_preactivation, content_vector, retention_slack, surge_rate):
    query_act = jax.nn.silu(probe_preactivation.astype(jnp.float32))
    admission_factor = retention_slack[None, :] * jax.nn.sigmoid(-retention_preactivation.astype(jnp.float32))
    retention_logarithm = jnp.log1p(-admission_factor) + surge_rate
    return (query_act, admission_factor, content_vector.astype(jnp.float32), retention_logarithm)

def head_output(outputs, subspace_scaling_factor, emission_preactivation):
    count, heads_here = (outputs.shape[0], outputs.shape[1])
    squares = lax.optimization_barrier(jnp.mean(outputs * outputs, axis=-1, keepdims=True))
    scaled = outputs * lax.rsqrt(squares + EPSILON) * subspace_scaling_factor.reshape(heads_here, HEAD_DIM)
    scaled = scaled.reshape(count, heads_here * HEAD_DIM)
    return (scaled * jax.nn.silu(emission_preactivation.astype(jnp.float32))).astype(jnp.bfloat16)

def row_norm(stream, mlp_scaling_factor):
    streamf = stream.astype(jnp.float32)
    squares = lax.optimization_barrier(jnp.mean(streamf * streamf, axis=-1, keepdims=True))
    return (streamf * lax.rsqrt(squares + EPSILON) * mlp_scaling_factor).astype(jnp.bfloat16)

def reference(skip_stream_vector, probe_preactivation, retention_preactivation, content_vector, emission_preactivation, retention_slack, surge_rate, subspace_scaling_factor, emission_matrix, mlp_scaling_factor, switch_matrix, expansion_matrix, contraction_matrix):
    arranged_sources = admission_source_matrix(probe_preactivation, retention_preactivation, content_vector, retention_slack, surge_rate)
    block_list = tuple((split_blocks(item, HEADS) for item in arranged_sources))
    start_carry = (jnp.zeros((HEADS, HEAD_DIM, HEAD_DIM), jnp.float32), jnp.zeros((HEADS, HEAD_DIM), jnp.float32))
    _, (outputs, _) = lax.scan(block_step, start_carry, block_list)
    outputs = outputs.transpose(0, 2, 1, 3).reshape(TOKENS, HEADS, HEAD_DIM)
    mixed = head_output(outputs, subspace_scaling_factor, emission_preactivation)
    projected = jnp.dot(mixed, emission_matrix, preferred_element_type=jnp.float32)
    stream = (skip_stream_vector.astype(jnp.float32) + projected).astype(jnp.bfloat16)
    normed = row_norm(stream, mlp_scaling_factor)
    gate_proj = jnp.dot(normed, switch_matrix, preferred_element_type=jnp.float32)
    up_proj = jnp.dot(normed, expansion_matrix, preferred_element_type=jnp.float32)
    hidden = (jax.nn.silu(gate_proj) * up_proj).astype(jnp.bfloat16)
    slice_width = FF // N_TP
    summed = jnp.zeros((TOKENS, D), jnp.float32)
    for member in range(N_TP):
        lower = member * slice_width
        partial_sum = jnp.dot(hidden[:, lower:lower + slice_width], contraction_matrix[lower:lower + slice_width], preferred_element_type=jnp.float32)
        summed = summed + partial_sum.astype(jnp.bfloat16).astype(jnp.float32)
    return (stream.astype(jnp.float32) + summed).astype(jnp.bfloat16)
```

```python
import functools

import jax
import jax.numpy as jnp
from jax import lax
from jax.experimental import pallas as pl
from jax.experimental.pallas import tpu as pltpu
from jax.sharding import PartitionSpec as P

HEAD_DIM = 128
BLOCK = 64
STATE_ROWS = HEAD_DIM + 16
EPSILON = 1e-06
MESH = pl.DeviceIdType.MESH
F32, BF16 = jnp.float32, jnp.bfloat16
LAST = (((1,), (1,)), ((), ()))
FIRST = (((0,), (0,)), ((), ()))


def weight_plan(n, me):
    every = (0, 1, 2)
    if n != 8:
        return [[(me, lax.rem(me + d, n), lax.rem(me + n - d, n), every) for d in range(1, n)]]
    ny, nz = 2, n // 2
    z, y = me // ny, lax.rem(me, ny)

    def at(dz, flip):
        return lax.rem(z + dz + nz, nz) * ny + (1 - y if flip else y)

    return [
        [
            (me, at(0, 1), at(0, 1), every),
            (me, at(1, 0), at(-1, 0), every),
            (me, at(-1, 0), at(1, 0), every),
        ],
        [
            (at(1, 0), at(0, 1), at(1, 1), every),
            (at(0, 1), at(1, 0), at(-1, 1), every),
            (at(1, 0), at(-1, 0), at(2, 0), every),
        ],
        [
            (at(2, 0), at(0, 1), at(2, 1), (0,)),
            (at(-1, 1), at(1, 0), at(2, 1), (1,)),
            (at(1, 1), at(-1, 0), at(2, 1), (2,)),
        ],
    ]


def kernel(
    n,
    m,
    skip_ref,
    query_ref,
    forget_ref,
    value_ref,
    emission_ref,
    slack_ref,
    surge_ref,
    gain_ref,
    projection_ref,
    row_gain_ref,
    switch_ref,
    expansion_ref,
    contraction_ref,
    out_ref,
    switch_all,
    expansion_all,
    contraction_all,
    projection,
    stream,
    normed,
    hidden,
    mixed,
    outputs,
    decayed_query,
    state,
    offset,
    state_out,
    state_in,
    part,
    from_buddy,
    cross_out,
    cross_in,
    local_sem,
    weight_send,
    weight_recv,
    skip_send,
    skip_recv,
    mixed_send,
    mixed_recv,
    state_send,
    state_recv,
    buddy_send,
    buddy_recv,
    cross_send,
    cross_recv,
):
    sp, tp = lax.axis_index("sp"), lax.axis_index("tp")
    tokens, width = query_ref.shape
    rows, model = skip_ref.shape
    depth, units = switch_ref.shape
    heads = width // HEAD_DIM
    pairs = m // 2

    barrier = pltpu.get_barrier_semaphore()
    for d in range(1, n):
        pl.semaphore_signal(barrier, inc=1, device_id=(lax.rem(sp + d, n), tp), device_id_type=MESH)
    for d in range(1, m):
        pl.semaphore_signal(barrier, inc=1, device_id=(sp, lax.rem(tp + d, m)), device_id_type=MESH)
    pl.semaphore_wait(barrier, n - 1 + m - 1)

    def remote(src, dst, send, recv, device):
        return pltpu.make_async_remote_copy(
            src_ref=src, dst_ref=dst, send_sem=send, recv_sem=recv, device_id=device, device_id_type=MESH
        )

    own_units = (switch_ref, expansion_ref, contraction_ref)

    def unit(tensor, owner):
        if tensor == 2:
            return contraction_all.at[owner]
        held = (switch_all, expansion_all)[tensor]
        return held.at[pl.ds(pl.multiple_of(owner * depth, depth), depth)]

    plan = weight_plan(n, sp)
    sends = []
    arrivals = []
    index = 0
    for number, step in enumerate(plan):
        sends.append([])
        arrivals.append([])
        for tensor in (0, 1, 2):
            for owner, target, arriving, tensors in step:
                if tensor not in tensors:
                    continue
                src = own_units[tensor] if number == 0 else unit(tensor, owner)
                args = (weight_send.at[index], weight_recv.at[index], (target, tp))
                sends[-1].append(remote(src, unit(tensor, owner), *args))
                arrivals[-1].append(remote(unit(tensor, arriving), unit(tensor, arriving), *args))
                index += 1

    for copy in sends[0]:
        copy.start()

    def rows_of(owner):
        return pl.ds(pl.multiple_of(owner * rows, rows), rows)

    skip_sends, skip_arrivals, mixed_sends, mixed_arrivals = [], [], [], []
    for d in range(1, m):
        source, target = lax.rem(tp + m - d, m), (sp, lax.rem(tp + d, m))
        sems = (skip_send.at[d - 1], skip_recv.at[d - 1], target)
        skip_sends.append(remote(skip_ref, stream.at[rows_of(tp)], *sems))
        skip_arrivals.append(remote(stream.at[rows_of(source)], stream.at[rows_of(source)], *sems))
        sems = (mixed_send.at[d - 1], mixed_recv.at[d - 1], target)
        mixed_sends.append(remote(mixed.at[tp], mixed.at[tp], *sems))
        mixed_arrivals.append(remote(mixed.at[source], mixed.at[source], *sems))
    for copy in skip_sends:
        copy.start()
    local = [
        pltpu.make_async_copy(skip_ref, stream.at[rows_of(tp)], local_sem.at[0]),
        pltpu.make_async_copy(projection_ref, projection, local_sem.at[1]),
    ] + [pltpu.make_async_copy(own_units[t], unit(t, sp), local_sem.at[2 + t]) for t in range(3)]
    for copy in local:
        copy.start()

    state[...] = jnp.zeros_like(state)
    offset[...] = jnp.zeros_like(offset)
    before = lax.broadcasted_iota(jnp.int32, (BLOCK, BLOCK), 0) >= lax.broadcasted_iota(
        jnp.int32, (BLOCK, BLOCK), 1
    )
    lower = before.astype(F32)

    @pl.loop(0, tokens // BLOCK)
    def _(block):
        here = pl.ds(pl.multiple_of(block * BLOCK, BLOCK), BLOCK)
        raw = query_ref[here, :].astype(F32)
        query = raw * jax.nn.sigmoid(raw)
        gate = slack_ref[...] * jax.nn.sigmoid(-forget_ref[here, :].astype(F32))
        log_forget = jnp.log1p(-gate) + surge_ref[here, :]
        total = jnp.dot(lower, log_forget, precision=lax.Precision.HIGHEST, preferred_element_type=F32)
        middle, last = total[BLOCK // 2 : BLOCK // 2 + 1, :], total[BLOCK - 1 :, :]
        left = (query * jnp.exp(total - middle)).astype(BF16)
        right = (gate * jnp.exp(middle - total)).astype(BF16)
        carried = (query * jnp.exp(total)).astype(BF16)
        kept = (gate * jnp.exp(last - total)).astype(BF16)
        decayed_query[here, :] = (query * jnp.exp(total + offset[...])).astype(BF16)
        closing = jnp.exp(last)
        for head in range(heads):
            lanes = slice(head * HEAD_DIM, (head + 1) * HEAD_DIM)
            value = value_ref[here, lanes]
            scores = lax.dot_general(left[:, lanes], right[:, lanes], LAST, preferred_element_type=F32)
            scores = jnp.where(before, scores, 0.0).astype(BF16)
            held = state[head]
            outputs[here, lanes] = jnp.dot(
                scores, value, preferred_element_type=F32
            ) + lax.dot_general(carried[:, lanes], held.astype(BF16), LAST, preferred_element_type=F32)
            state[head] = closing[:, lanes] * held + lax.dot_general(
                value, kept[:, lanes], FIRST, preferred_element_type=F32
            )
        offset[...] += last

    for head in range(heads):
        lanes = slice(head * HEAD_DIM, (head + 1) * HEAD_DIM)
        state_out[head, :HEAD_DIM, :] = state[head].astype(BF16)
        decay = jnp.exp(offset[:, lanes])
        state_out[head, HEAD_DIM:, :] = jnp.broadcast_to(decay, (16, HEAD_DIM)).astype(BF16)
    state_copies = []
    for d in range(1, n):
        copy = remote(
            state_out,
            state_in.at[d - 1],
            state_send.at[d - 1],
            state_recv.at[d - 1],
            (lax.rem(sp + d, n), tp),
        )
        state_copies.append(copy)
        pl.when(sp + d < n)(copy.start)

    if len(plan) > 1:
        for copy in arrivals[0]:
            copy.wait_recv()
        for copy in sends[1]:
            copy.start()

    for d in range(1, n):
        pl.when(sp >= d)(state_copies[d - 1].wait_recv)
    state[...] = jnp.zeros_like(state)

    @pl.loop(0, sp)
    def _(earlier):
        slot = sp - earlier - 1
        for head in range(heads):
            item = state_in[slot, head].astype(F32)
            state[head] = item[HEAD_DIM : HEAD_DIM + 1, :] * state[head] + item[:HEAD_DIM, :]

    tile = min(256, tokens)

    @pl.loop(0, tokens // tile)
    def _(turn):
        here = pl.ds(pl.multiple_of(turn * tile, tile), tile)
        for head in range(heads):
            lanes = slice(head * HEAD_DIM, (head + 1) * HEAD_DIM)
            full = outputs[here, lanes] + lax.dot_general(
                decayed_query[here, lanes], state[head].astype(BF16), LAST, preferred_element_type=F32
            )
            squares = jnp.mean(full * full, axis=-1, keepdims=True)
            raw = emission_ref[here, lanes].astype(F32)
            scaled = full * lax.rsqrt(squares + EPSILON) * gain_ref[:, lanes]
            mixed[tp, here, lanes] = (scaled * (raw * jax.nn.sigmoid(raw))).astype(BF16)

    for copy in mixed_sends:
        copy.start()
    for copy in local:
        copy.wait()
    for copy in skip_arrivals:
        copy.wait_recv()
    for copy in mixed_arrivals:
        copy.wait_recv()

    @pl.loop(0, tokens // tile)
    def _(turn):
        here = pl.ds(pl.multiple_of(turn * tile, tile), tile)
        total = stream[here, :].astype(F32)
        for source in range(m):
            total += jnp.dot(
                mixed[source, here, :],
                projection[source * width : (source + 1) * width, :],
                preferred_element_type=F32,
            )
        rounded = total.astype(BF16)
        stream[here, :] = rounded
        total = rounded.astype(F32)
        squares = jnp.mean(total * total, axis=-1, keepdims=True)
        normed[here, :] = (total * lax.rsqrt(squares + EPSILON) * row_gain_ref[...]).astype(BF16)

    if len(plan) > 1:
        for copy in arrivals[1]:
            copy.wait_recv()
        for copy in sends[2]:
            copy.start()
    for copy in arrivals[-1]:
        copy.wait_recv()

    core, pair = lax.rem(tp, 2), tp // 2
    buddy = (sp, pair * 2 + 1 - core)

    def half(number, which):
        return part.at[number, pl.ds(pl.multiple_of(which * rows, rows), rows)]

    def feed_forward(number, owner):
        inputs = pl.ds(pl.multiple_of(owner * 2 * rows, 2 * rows), 2 * rows)

        def columns(lanes):
            value = normed[inputs, :]
            gate = jnp.dot(value, switch_all[:, lanes], preferred_element_type=F32)
            up = jnp.dot(value, expansion_all[:, lanes], preferred_element_type=F32)
            hidden[:, lanes] = (gate * jax.nn.sigmoid(gate) * up).astype(BF16)

        @pl.loop(0, units // 256)
        def _(turn):
            columns(pl.ds(pl.multiple_of(turn * 256, 256), 256))

        if units % 256:
            columns(slice(units // 256 * 256, units))

        @pl.loop(0, n)
        def _(turn):
            lanes = pl.ds(pl.multiple_of(turn * depth, depth), depth)
            part[number, :, lanes] = jnp.dot(
                hidden[...], contraction_all[turn], preferred_element_type=F32
            ).astype(BF16)

        copy = remote(
            half(number, 1 - core),
            from_buddy.at[number],
            buddy_send.at[number],
            buddy_recv.at[number],
            buddy,
        )
        copy.start()
        return copy

    tail = []
    for d in range(1, pairs):
        owner = lax.rem(pair + d, pairs)
        copy = feed_forward(d, owner)
        copy.wait_recv()
        cross_out[d - 1] = (half(d, core)[...].astype(F32) + from_buddy[d].astype(F32)).astype(BF16)
        cross = remote(
            cross_out.at[d - 1],
            cross_in.at[d - 1],
            cross_send.at[d - 1],
            cross_recv.at[d - 1],
            (sp, owner * 2 + core),
        )
        cross.start()
        tail += [copy, cross]
    copy = feed_forward(0, pair)
    copy.wait_recv()
    total = half(0, core)[...].astype(F32) + from_buddy[0].astype(F32) + stream[rows_of(tp), :].astype(F32)
    for d in range(1, pairs):
        tail[2 * d - 1].wait_recv()
        total += cross_in[d - 1].astype(F32)
    out_ref[...] = total.astype(BF16)

    for copy in tail + [copy] + skip_sends + mixed_sends + [c for step in sends for c in step]:
        copy.wait_send()
    for d in range(1, n):
        pl.when(sp + d < n)(state_copies[d - 1].wait_send)


def on_device(n, m, *arrays):
    (skip, query, forget, value, emission, slack, surge, gain, projection, row_gain, switch, expansion, contraction) = arrays
    tokens, width = query.shape
    rows, model = skip.shape
    depth, units = switch.shape
    heads, pairs = width // HEAD_DIM, m // 2
    count = 21 if n == 8 else 3 * (n - 1)
    vmem, anywhere = pl.BlockSpec(memory_space=pltpu.VMEM), pl.BlockSpec(memory_space=pl.ANY)
    dma = pltpu.SemaphoreType.DMA
    return pl.pallas_call(
        functools.partial(kernel, n, m),
        out_shape=jax.ShapeDtypeStruct((rows, model), BF16),
        in_specs=[anywhere] + [vmem] * 7 + [anywhere, vmem] + [anywhere] * 3,
        out_specs=vmem,
        scratch_shapes=[
            pltpu.VMEM((model, units), BF16),
            pltpu.VMEM((model, units), BF16),
            pltpu.VMEM((n, units, depth), BF16),
            pltpu.VMEM(projection.shape, BF16),
            pltpu.VMEM((tokens, model), BF16),
            pltpu.VMEM((tokens, model), BF16),
            pltpu.VMEM((2 * rows, units), BF16),
            pltpu.VMEM((m, tokens, width), BF16),
            pltpu.VMEM((tokens, width), F32),
            pltpu.VMEM((tokens, width), BF16),
            pltpu.VMEM((heads, HEAD_DIM, HEAD_DIM), F32),
            pltpu.VMEM((1, width), F32),
            pltpu.VMEM((heads, STATE_ROWS, HEAD_DIM), BF16),
            pltpu.VMEM((n - 1, heads, STATE_ROWS, HEAD_DIM), BF16),
            pltpu.VMEM((pairs, 2 * rows, model), BF16),
            pltpu.VMEM((pairs, rows, model), BF16),
            pltpu.VMEM((pairs - 1, rows, model), BF16),
            pltpu.VMEM((pairs - 1, rows, model), BF16),
            dma((5,)),
            dma((count,)),
            dma((count,)),
            dma((m - 1,)),
            dma((m - 1,)),
            dma((m - 1,)),
            dma((m - 1,)),
            dma((n - 1,)),
            dma((n - 1,)),
            dma((pairs,)),
            dma((pairs,)),
            dma((pairs - 1,)),
            dma((pairs - 1,)),
        ],
        compiler_params=pltpu.CompilerParams(
            collective_id=0, has_side_effects=True, vmem_limit_bytes=63_000_000
        ),
    )(
        skip,
        query,
        forget,
        value,
        emission,
        slack.reshape(1, width),
        surge,
        gain.reshape(1, width),
        projection,
        row_gain.reshape(1, model),
        switch,
        expansion,
        contraction,
    )


def solution(mesh):
    in_specs = (
        P(("sp", "tp"), None),
        P("sp", "tp"),
        P("sp", "tp"),
        P("sp", "tp"),
        P("sp", "tp"),
        P("tp"),
        P("sp", "tp"),
        P("tp"),
        P(),
        P(),
        P("sp", "tp"),
        P("sp", "tp"),
        P("tp", "sp"),
    )
    return jax.shard_map(
        functools.partial(on_device, mesh.shape["sp"], mesh.shape["tp"]),
        mesh=mesh,
        in_specs=in_specs,
        out_specs=P(("sp", "tp"), None),
        check_vma=False,
    )
```

```python
import functools

import jax
import jax.numpy as jnp
from jax import lax
from jax.experimental import pallas as pl
from jax.experimental.pallas import tpu as pltpu
from jax.sharding import PartitionSpec as P

HEAD_DIM = 128
BLOCK = 64
STATE_ROWS = HEAD_DIM + 16
EPSILON = 1e-06
MESH = pl.DeviceIdType.MESH
F32, BF16 = jnp.float32, jnp.bfloat16
LAST = (((1,), (1,)), ((), ()))
FIRST = (((0,), (0,)), ((), ()))


def weight_plan(n, me):
    out = []
    if n != 8:
        for tensor in range(3):
            for d in range(1, n):
                to, source = lax.rem(me + d, n), lax.rem(me + n - d, n)
                out.append((0, tensor, ("D", d, tensor), True, me, to, True, source, None))
        return out
    ny, nz = 2, n // 2
    z, y = me // ny, lax.rem(me, ny)

    def at(place, flip):
        return jnp.clip(place, 0, nz - 1) * ny + (1 - y if flip else y)

    def crossed(place, tensor, way):
        first, last = (1, nz - 1) if way > 0 else (nz - 2, 0)
        return (place == first) | (place == last) if tensor == 0 else place == first

    def inside(place):
        return (place >= 0) & (place < nz)

    for tensor in range(3):
        late = 1 if tensor == 2 else 0
        out.append((0, tensor, ("Y", 0, tensor), True, me, at(z, 1), True, at(z, 1), None))
        for way in (1, -1):
            for k in range(1, nz):
                to, unit = z + way, z + way - way * k
                name, above = (way, k, tensor), (way, k - 1, tensor)
                stage = 0 if k == 1 else k - 1 + late
                out.append(
                    (stage, tensor, name, inside(to) & inside(unit), at(unit, 0), at(to, 0),
                     inside(z - way * k), at(z - way * k, 0), None if k == 1 else above)
                )
                held = inside(z - way * k)
                if k == 1:
                    held = held & jnp.logical_not(crossed(z, tensor, way))
                out.append(
                    (k + late, tensor, ("Y", way * k, tensor), held, at(z - way * k, 0), at(z, 1),
                     held, at(z - way * k, 1), name)
                )
            out.append(
                (2, tensor, ("X", way, tensor), inside(z + way) & crossed(z + way, tensor, way), at(z, 1),
                 at(z + way, 0), crossed(z, tensor, way), at(z - way, 1), ("Y", 0, tensor))
            )
    return out


def kernel(
    n,
    m,
    skip_ref,
    query_ref,
    forget_ref,
    value_ref,
    emission_ref,
    slack_ref,
    surge_ref,
    gain_ref,
    projection_ref,
    row_gain_ref,
    switch_ref,
    expansion_ref,
    contraction_ref,
    out_ref,
    switch_all,
    expansion_all,
    contraction_all,
    projection,
    stream,
    normed,
    hidden,
    mixed,
    outputs,
    decayed_query,
    state,
    offset,
    state_out,
    state_in,
    part,
    from_buddy,
    cross_out,
    cross_in,
    local_sem,
    weight_send,
    weight_recv,
    skip_send,
    skip_recv,
    mixed_send,
    mixed_recv,
    state_send,
    state_recv,
    buddy_send,
    buddy_recv,
    cross_send,
    cross_recv,
):
    sp, tp = lax.axis_index("sp"), lax.axis_index("tp")
    tokens, width = query_ref.shape
    rows, model = skip_ref.shape
    depth, units = switch_ref.shape
    heads = width // HEAD_DIM
    pairs = m // 2

    barrier = pltpu.get_barrier_semaphore()
    for d in range(1, n):
        pl.semaphore_signal(barrier, inc=1, device_id=(lax.rem(sp + d, n), tp), device_id_type=MESH)
    for d in range(1, m):
        pl.semaphore_signal(barrier, inc=1, device_id=(sp, lax.rem(tp + d, m)), device_id_type=MESH)
    pl.semaphore_wait(barrier, n - 1 + m - 1)

    def remote(src, dst, send, recv, device):
        return pltpu.make_async_remote_copy(
            src_ref=src, dst_ref=dst, send_sem=send, recv_sem=recv, device_id=device, device_id_type=MESH
        )

    own_units = (switch_ref, expansion_ref, contraction_ref)

    def unit(tensor, owner):
        if tensor == 2:
            return contraction_all.at[owner]
        held = (switch_all, expansion_all)[tensor]
        return held.at[pl.ds(pl.multiple_of(owner * depth, depth), depth)]

    messages = {}
    for index, (stage, tensor, name, sent, owner, target, arrives, arriving, after) in enumerate(
        weight_plan(n, sp)
    ):
        src = own_units[tensor] if stage == 0 else unit(tensor, owner)
        args = (weight_send.at[index], weight_recv.at[index], (target, tp))
        send = remote(src, unit(tensor, owner), *args)
        arrival = remote(unit(tensor, arriving), unit(tensor, arriving), *args)
        messages[name] = (stage, sent, send, arrives, arrival, after)
    arrived = set()

    def where(condition, action):
        if condition is True:
            action()
        else:
            pl.when(condition)(action)

    def await_unit(name):
        if name not in arrived:
            arrived.add(name)
            where(messages[name][3], messages[name][4].wait_recv)

    def run_stage(wanted):
        for name, (stage, sent, send, _, _, after) in messages.items():
            if stage == wanted:
                if after is not None:
                    await_unit(after)
                where(sent, send.start)

    run_stage(0)

    def rows_of(owner):
        return pl.ds(pl.multiple_of(owner * rows, rows), rows)

    skip_sends, skip_arrivals, mixed_sends, mixed_arrivals = [], [], [], []
    for d in range(1, m):
        source, target = lax.rem(tp + m - d, m), (sp, lax.rem(tp + d, m))
        sems = (skip_send.at[d - 1], skip_recv.at[d - 1], target)
        skip_sends.append(remote(skip_ref, stream.at[rows_of(tp)], *sems))
        skip_arrivals.append(remote(stream.at[rows_of(source)], stream.at[rows_of(source)], *sems))
        sems = (mixed_send.at[d - 1], mixed_recv.at[d - 1], target)
        mixed_sends.append(remote(mixed.at[tp], mixed.at[tp], *sems))
        mixed_arrivals.append(remote(mixed.at[source], mixed.at[source], *sems))
    for copy in skip_sends:
        copy.start()
    local = [
        pltpu.make_async_copy(skip_ref, stream.at[rows_of(tp)], local_sem.at[0]),
        pltpu.make_async_copy(projection_ref, projection, local_sem.at[1]),
    ] + [pltpu.make_async_copy(own_units[t], unit(t, sp), local_sem.at[2 + t]) for t in range(3)]
    for copy in local:
        copy.start()

    state[...] = jnp.zeros_like(state)
    offset[...] = jnp.zeros_like(offset)
    before = lax.broadcasted_iota(jnp.int32, (BLOCK, BLOCK), 0) >= lax.broadcasted_iota(
        jnp.int32, (BLOCK, BLOCK), 1
    )
    lower = before.astype(F32)

    @pl.loop(0, tokens // BLOCK)
    def _(block):
        here = pl.ds(pl.multiple_of(block * BLOCK, BLOCK), BLOCK)
        raw = query_ref[here, :].astype(F32)
        query = raw * jax.nn.sigmoid(raw)
        gate = slack_ref[...] * jax.nn.sigmoid(-forget_ref[here, :].astype(F32))
        log_forget = jnp.log1p(-gate) + surge_ref[here, :]
        total = jnp.dot(lower, log_forget, precision=lax.Precision.HIGHEST, preferred_element_type=F32)
        middle, last = total[BLOCK // 2 : BLOCK // 2 + 1, :], total[BLOCK - 1 :, :]
        left = (query * jnp.exp(total - middle)).astype(BF16)
        right = (gate * jnp.exp(middle - total)).astype(BF16)
        carried = (query * jnp.exp(total)).astype(BF16)
        kept = (gate * jnp.exp(last - total)).astype(BF16)
        decayed_query[here, :] = (query * jnp.exp(total + offset[...])).astype(BF16)
        closing = jnp.exp(last)
        for head in range(heads):
            lanes = slice(head * HEAD_DIM, (head + 1) * HEAD_DIM)
            value = value_ref[here, lanes]
            scores = lax.dot_general(left[:, lanes], right[:, lanes], LAST, preferred_element_type=F32)
            scores = jnp.where(before, scores, 0.0).astype(BF16)
            held = state[head]
            outputs[here, lanes] = jnp.dot(
                scores, value, preferred_element_type=F32
            ) + lax.dot_general(carried[:, lanes], held.astype(BF16), LAST, preferred_element_type=F32)
            state[head] = closing[:, lanes] * held + lax.dot_general(
                value, kept[:, lanes], FIRST, preferred_element_type=F32
            )
        offset[...] += last

    for head in range(heads):
        lanes = slice(head * HEAD_DIM, (head + 1) * HEAD_DIM)
        state_out[head, :HEAD_DIM, :] = state[head].astype(BF16)
        decay = jnp.exp(offset[:, lanes])
        state_out[head, HEAD_DIM:, :] = jnp.broadcast_to(decay, (16, HEAD_DIM)).astype(BF16)
    state_copies = []
    for d in range(1, n):
        copy = remote(
            state_out,
            state_in.at[d - 1],
            state_send.at[d - 1],
            state_recv.at[d - 1],
            (lax.rem(sp + d, n), tp),
        )
        state_copies.append(copy)
        pl.when(sp + d < n)(copy.start)

    run_stage(1)

    for d in range(1, n):
        pl.when(sp >= d)(state_copies[d - 1].wait_recv)
    state[...] = jnp.zeros_like(state)

    @pl.loop(0, sp)
    def _(earlier):
        slot = sp - earlier - 1
        for head in range(heads):
            item = state_in[slot, head].astype(F32)
            state[head] = item[HEAD_DIM : HEAD_DIM + 1, :] * state[head] + item[:HEAD_DIM, :]

    tile = min(256, tokens)

    @pl.loop(0, tokens // tile)
    def _(turn):
        here = pl.ds(pl.multiple_of(turn * tile, tile), tile)
        for head in range(heads):
            lanes = slice(head * HEAD_DIM, (head + 1) * HEAD_DIM)
            full = outputs[here, lanes] + lax.dot_general(
                decayed_query[here, lanes], state[head].astype(BF16), LAST, preferred_element_type=F32
            )
            squares = jnp.mean(full * full, axis=-1, keepdims=True)
            raw = emission_ref[here, lanes].astype(F32)
            scaled = full * lax.rsqrt(squares + EPSILON) * gain_ref[:, lanes]
            mixed[tp, here, lanes] = (scaled * (raw * jax.nn.sigmoid(raw))).astype(BF16)

    for copy in mixed_sends:
        copy.start()
    run_stage(2)
    for copy in local:
        copy.wait()
    for copy in skip_arrivals:
        copy.wait_recv()
    for copy in mixed_arrivals:
        copy.wait_recv()

    @pl.loop(0, tokens // tile)
    def _(turn):
        here = pl.ds(pl.multiple_of(turn * tile, tile), tile)
        total = stream[here, :].astype(F32)
        for source in range(m):
            total += jnp.dot(
                mixed[source, here, :],
                projection[source * width : (source + 1) * width, :],
                preferred_element_type=F32,
            )
        rounded = total.astype(BF16)
        stream[here, :] = rounded
        total = rounded.astype(F32)
        squares = jnp.mean(total * total, axis=-1, keepdims=True)
        normed[here, :] = (total * lax.rsqrt(squares + EPSILON) * row_gain_ref[...]).astype(BF16)

    run_stage(3)
    for name in messages:
        if name[2] < 2:
            await_unit(name)

    core, pair = lax.rem(tp, 2), tp // 2
    buddy = (sp, pair * 2 + 1 - core)

    def half(number, which):
        return part.at[number, pl.ds(pl.multiple_of(which * rows, rows), rows)]

    def gate_and_up(number, owner):
        inputs = pl.ds(pl.multiple_of(owner * 2 * rows, 2 * rows), 2 * rows)

        def columns(lanes):
            value = normed[inputs, :]
            gate = jnp.dot(value, switch_all[:, lanes], preferred_element_type=F32)
            up = jnp.dot(value, expansion_all[:, lanes], preferred_element_type=F32)
            hidden[number, :, lanes] = (gate * jax.nn.sigmoid(gate) * up).astype(BF16)

        @pl.loop(0, units // 256)
        def _(turn):
            columns(pl.ds(pl.multiple_of(turn * 256, 256), 256))

        if units % 256:
            columns(slice(units // 256 * 256, units))

    def down(number):
        @pl.loop(0, n)
        def _(turn):
            lanes = pl.ds(pl.multiple_of(turn * depth, depth), depth)
            part[number, :, lanes] = jnp.dot(
                hidden[number], contraction_all[turn], preferred_element_type=F32
            ).astype(BF16)

        copy = remote(
            half(number, 1 - core),
            from_buddy.at[number],
            buddy_send.at[number],
            buddy_recv.at[number],
            buddy,
        )
        copy.start()
        return copy

    for d in [*range(1, pairs), 0]:
        gate_and_up(d, lax.rem(pair + d, pairs))
    run_stage(4)
    for name in messages:
        await_unit(name)
    tail = []
    for d in range(1, pairs):
        owner = lax.rem(pair + d, pairs)
        copy = down(d)
        copy.wait_recv()
        cross_out[d - 1] = (half(d, core)[...].astype(F32) + from_buddy[d].astype(F32)).astype(BF16)
        cross = remote(
            cross_out.at[d - 1],
            cross_in.at[d - 1],
            cross_send.at[d - 1],
            cross_recv.at[d - 1],
            (sp, owner * 2 + core),
        )
        cross.start()
        tail += [copy, cross]
    copy = down(0)
    copy.wait_recv()
    total = half(0, core)[...].astype(F32) + from_buddy[0].astype(F32) + stream[rows_of(tp), :].astype(F32)
    for d in range(1, pairs):
        tail[2 * d - 1].wait_recv()
        total += cross_in[d - 1].astype(F32)
    out_ref[...] = total.astype(BF16)

    for copy in tail + [copy] + skip_sends + mixed_sends:
        copy.wait_send()
    for _, sent, send, _, _, _ in messages.values():
        where(sent, send.wait_send)
    for d in range(1, n):
        pl.when(sp + d < n)(state_copies[d - 1].wait_send)


def on_device(n, m, *arrays):
    (skip, query, forget, value, emission, slack, surge, gain, projection, row_gain, switch, expansion, contraction) = arrays
    tokens, width = query.shape
    rows, model = skip.shape
    depth, units = switch.shape
    heads, pairs = width // HEAD_DIM, m // 2
    count = 3 * (3 * n // 2 + 3) if n == 8 else 3 * (n - 1)
    vmem, anywhere = pl.BlockSpec(memory_space=pltpu.VMEM), pl.BlockSpec(memory_space=pl.ANY)
    dma = pltpu.SemaphoreType.DMA
    return pl.pallas_call(
        functools.partial(kernel, n, m),
        out_shape=jax.ShapeDtypeStruct((rows, model), BF16),
        in_specs=[anywhere] + [vmem] * 7 + [anywhere, vmem] + [anywhere] * 3,
        out_specs=vmem,
        scratch_shapes=[
            pltpu.VMEM((model, units), BF16),
            pltpu.VMEM((model, units), BF16),
            pltpu.VMEM((n, units, depth), BF16),
            pltpu.VMEM(projection.shape, BF16),
            pltpu.VMEM((tokens, model), BF16),
            pltpu.VMEM((tokens, model), BF16),
            pltpu.VMEM((pairs, 2 * rows, units), BF16),
            pltpu.VMEM((m, tokens, width), BF16),
            pltpu.VMEM((tokens, width), F32),
            pltpu.VMEM((tokens, width), BF16),
            pltpu.VMEM((heads, HEAD_DIM, HEAD_DIM), F32),
            pltpu.VMEM((1, width), F32),
            pltpu.VMEM((heads, STATE_ROWS, HEAD_DIM), BF16),
            pltpu.VMEM((n - 1, heads, STATE_ROWS, HEAD_DIM), BF16),
            pltpu.VMEM((pairs, 2 * rows, model), BF16),
            pltpu.VMEM((pairs, rows, model), BF16),
            pltpu.VMEM((pairs - 1, rows, model), BF16),
            pltpu.VMEM((pairs - 1, rows, model), BF16),
            dma((5,)),
            dma((count,)),
            dma((count,)),
            dma((m - 1,)),
            dma((m - 1,)),
            dma((m - 1,)),
            dma((m - 1,)),
            dma((n - 1,)),
            dma((n - 1,)),
            dma((pairs,)),
            dma((pairs,)),
            dma((pairs - 1,)),
            dma((pairs - 1,)),
        ],
        compiler_params=pltpu.CompilerParams(
            collective_id=0, has_side_effects=True, vmem_limit_bytes=63_000_000
        ),
    )(
        skip,
        query,
        forget,
        value,
        emission,
        slack.reshape(1, width),
        surge,
        gain.reshape(1, width),
        projection,
        row_gain.reshape(1, model),
        switch,
        expansion,
        contraction,
    )


def solution(mesh):
    in_specs = (
        P(("sp", "tp"), None),
        P("sp", "tp"),
        P("sp", "tp"),
        P("sp", "tp"),
        P("sp", "tp"),
        P("tp"),
        P("sp", "tp"),
        P("tp"),
        P(),
        P(),
        P("sp", "tp"),
        P("sp", "tp"),
        P("tp", "sp"),
    )
    return jax.shard_map(
        functools.partial(on_device, mesh.shape["sp"], mesh.shape["tp"]),
        mesh=mesh,
        in_specs=in_specs,
        out_specs=P(("sp", "tp"), None),
        check_vma=False,
    )
```
